32 devices in a mesh: sp: 8 (over z, x), tp: 4 (over y, core).
Axes of the slice: x: 2, y: 2, z: 4, core: 2. Of those that a mesh axis runs over, the one named last changes fastest.
Arguments:
- tokens: bfloat16 [4096, 2048], P(('sp', 'tp')), may hold values from -6 to 6
- elapsed: float32 [4096], P(('sp', 'tp')), may hold values from 0 to 3, as said below
- norm_gain: float32 [2048], replicated, may hold values from 0.1 to 1.9
- in_weight: bfloat16 [2048, 1024], replicated, may hold values from -0.125 to 0.125
- state_input: bfloat16 [2, 2, 64, 64, 16], replicated, may hold values from -1.5 to 1.5
- state_output: float32 [2, 2, 64, 16, 64], replicated, may hold values from -0.375 to 0.375
- forget_rate: float32 [2, 64, 64], replicated, may hold values from 0 to 1, as said below
- decay_angle: float32 [2, 64, 64], replicated, may hold values from -3.140625 to 3.140625
- skip_gain: float32 [1024], replicated, may hold values from -4 to 4
- glu_weight: bfloat16 [1024, 1024], replicated, may hold values from -0.1875 to 0.1875
- glu_bias: float32 [1024], replicated, may hold values from -4 to 4
- out_weight: bfloat16 [1024, 2048], replicated, may hold values from -0.1875 to 0.1875
- out_gain: float32 [2048], replicated, may hold values from 0.1 to 1.9
Outputs:
- mixed: bfloat16 [4096, 2048], P(('sp', 'tp'))
The draws below stay inside these ranges and needn't reach their ends.
Inputs may be any that keep to these rules, and one draw needn't show every extreme that they name: `elapsed`: positive time steps. `forget_rate`: positive rates.
All inputs are finite; a program needn't handle non-finite values.
Results may differ from the reference program's by a relative error of at most 0.0067.
Values sent between devices are 32-bit elements; how exact they have to be, the bound alone decides.
A program may use at most 128 MiB of HBM per device.

```python
import math
import jax
import jax.numpy as jnp
from jax import lax

D = 2048
GROUPS = 64
WIDTH = 16
STATE = 64
CHANNELS = 1024
TOK_DEV = 128
SEQ = 4096


def draw_elapsed(key, part):
    first_key, second_key = jax.random.split(key)
    factor = jnp.exp(jax.random.uniform(first_key, (64,), jnp.float32, math.log(0.5), math.log(2.0)))
    jitter = jax.random.uniform(second_key, (SEQ,), jnp.float32, 0.7, 1.4)
    return jnp.repeat(factor, SEQ // 64, total_repeat_length=SEQ) * jitter


def draw_forget_rate(key, part):
    pick_key, quick_key, slow_key = jax.random.split(key, 3)
    share = 0.5
    quick_groups = jax.random.bernoulli(pick_key, share, (2, GROUPS, 1))
    quick = jnp.exp(jax.random.uniform(quick_key, (2, GROUPS, STATE), jnp.float32, math.log(1.0 / 100.0), math.log(1.0 / 30.0)))
    slow = jnp.exp(jax.random.uniform(slow_key, (2, GROUPS, STATE), jnp.float32, math.log(0.05 / SEQ), math.log(2.0 / SEQ)))
    return jnp.where(quick_groups, quick, slow)


def steps_of(stream_key, shape, cuts, low, top_value):
    def one(position, shards_of):
        steps = jax.random.uniform(jax.random.fold_in(jax.random.fold_in(stream_key, 6), position), (shards_of,), jnp.float32, low / len(cuts), top_value / len(cuts))
        return jnp.repeat(jnp.exp(steps), shape[position] // shards_of).reshape((-1,) + (1,) * (len(shape) - position - 1))

    gain = one(*cuts[0])
    for cut in cuts[1:]:
        gain = gain * one(*cut)
    return gain


def centred(key, extent, deviation, reach, pieces=(), dtype=jnp.bfloat16):
    loudness = steps_of(key, extent, pieces, -0.22, 0.18) if pieces else 1.0
    values = jax.random.normal(key, extent, jnp.float32) * deviation * loudness
    return jnp.minimum(jnp.maximum(values, -reach), reach).astype(dtype)


def setup_inputs(seed: int = 0) -> dict:
    splits = jax.random.split(jax.random.key(seed), 14)
    tokens = centred(splits[0], (SEQ, D), 1.0, 6.0, ((0, 32),))
    elapsed = draw_elapsed(jax.random.fold_in(splits[13], 71), 0)
    norm_gain = jnp.clip(1.0 + 0.18 * jax.random.normal(splits[2], (D,), jnp.float32), 0.1, 1.9)
    in_weight = centred(splits[3], (D, CHANNELS), D ** -0.5, 0.125)
    state_input = centred(splits[4], (2, 2, GROUPS, STATE, WIDTH), WIDTH ** -0.5, 1.5)
    state_output = centred(splits[5], (2, 2, GROUPS, WIDTH, STATE), (4 * STATE) ** -0.5, 0.375, (), jnp.float32)
    forget_rate = draw_forget_rate(jax.random.fold_in(splits[13], 71), 0)
    decay_angle = jnp.clip(jax.random.uniform(splits[7], (2, GROUPS, STATE), jnp.float32, -3.140625, 3.140625), -3.140625, 3.140625)
    skip_gain = centred(splits[8], (CHANNELS,), 1.0, 4.0, (), jnp.float32)
    glu_weight = centred(splits[9], (CHANNELS, CHANNELS), CHANNELS ** -0.5, 0.1875)
    glu_bias = centred(splits[10], (CHANNELS,), 1.0, 4.0, (), jnp.float32)
    out_weight = centred(splits[11], (CHANNELS, D), CHANNELS ** -0.5, 0.1875)
    out_gain = jnp.clip(1.0 + 0.18 * jax.random.normal(splits[12], (D,), jnp.float32), 0.1, 1.9)
    return dict(tokens=tokens, elapsed=elapsed, norm_gain=norm_gain, in_weight=in_weight, state_input=state_input, state_output=state_output, forget_rate=forget_rate, decay_angle=decay_angle, skip_gain=skip_gain, glu_weight=glu_weight, glu_bias=glu_bias, out_weight=out_weight, out_gain=out_gain)


epsilon = 1e-06

def rms_scale(activations, gain_row):
    values = activations.astype(jnp.float32)
    return values * lax.rsqrt(lax.optimization_barrier(jnp.mean(values * values, axis=-1, keepdims=True)) + epsilon) * gain_row

def read_out(state_re, state_im, readout):
    count = state_re.shape[0]
    groups, group_width, states = (readout.shape[1], readout.shape[2], readout.shape[3])
    real_part = jnp.einsum('tgp,ghp->tgh', state_re.reshape(count, groups, states), readout[0], precision=lax.Precision.HIGHEST)
    imag_part = jnp.einsum('tgp,ghp->tgh', state_im.reshape(count, groups, states), readout[1], precision=lax.Precision.HIGHEST)
    return (real_part - imag_part).reshape(count, groups * group_width)

def direction_pass(driven, elapsed, inputs, readout, rate, angle, backward):
    cell_count = rate.shape[0]

    def block_step(state, piece):
        block_rows, block_steps = piece
        grouped = block_rows.astype(jnp.float32).reshape(TOK_DEV, GROUPS, WIDTH)
        proj_re = jnp.einsum('tgh,gph->tgp', grouped, inputs[0]).reshape(TOK_DEV, cell_count)
        proj_im = jnp.einsum('tgh,gph->tgp', grouped, inputs[1]).reshape(TOK_DEV, cell_count)
        steps_col = block_steps[:, None]
        damping = jnp.sqrt(-jnp.expm1(-2.0 * rate * steps_col))
        fade = jnp.exp(-rate * steps_col)
        angles = angle * steps_col
        decay_re = fade * jnp.cos(angles)
        decay_im = fade * jnp.sin(angles)

        def token_step(carry, item):
            old_re, old_im = carry
            step_re, step_im, push_re, push_im = item
            new_re = step_re * old_re - step_im * old_im + push_re
            new_im = step_re * old_im + step_im * old_re + push_im
            return ((new_re, new_im), (new_re, new_im))
        state, outputs = lax.scan(token_step, state, (decay_re, decay_im, proj_re * damping, proj_im * damping), reverse=backward)
        return (state, read_out(outputs[0], outputs[1], readout))
    start = (jnp.zeros((cell_count,), jnp.float32), jnp.zeros((cell_count,), jnp.float32))
    _, result = lax.scan(block_step, start, (driven, elapsed), reverse=backward)
    return result

def reference(tokens, elapsed, norm_gain, in_weight, state_input, state_output, forget_rate, decay_angle, skip_gain, glu_weight, glu_bias, out_weight, out_gain):
    normed = rms_scale(tokens, norm_gain).astype(jnp.bfloat16)
    driven = jnp.dot(normed, in_weight, preferred_element_type=jnp.float32).astype(jnp.bfloat16)
    response = skip_gain * driven.astype(jnp.float32)
    block_count = SEQ // TOK_DEV
    for direction in range(2):
        part_out = direction_pass(driven.reshape(block_count, TOK_DEV, CHANNELS), elapsed.reshape(block_count, TOK_DEV), state_input[direction].astype(jnp.float32), state_output[direction], forget_rate[direction].reshape(-1), decay_angle[direction].reshape(-1), direction == 1)
        response = response + part_out.reshape(SEQ, CHANNELS)
    active = jax.nn.gelu(response)
    gate_pre = jnp.dot(active.astype(jnp.bfloat16), glu_weight, preferred_element_type=jnp.float32) + glu_bias
    gated = (active * jax.nn.sigmoid(gate_pre)).astype(jnp.bfloat16)
    projected = jnp.dot(gated, out_weight, preferred_element_type=jnp.float32)
    return rms_scale(projected, out_gain).astype(jnp.bfloat16)
```

```python
import functools
import math

import jax
import jax.numpy as jnp
from jax import lax
from jax.experimental import pallas as pl
from jax.experimental.pallas import tpu as pltpu
from jax.sharding import PartitionSpec as P

epsilon = 1e-06
LANES = 128
SUB = 8
SIN = (4.44288292, -7.30824569, 3.60635422, -0.84611165, 0.10982452)
COS = (1.41421356, -6.97886411, 5.73988154, -1.88827492, 0.33225154, -0.03450161)
F32 = jnp.float32
BF16 = jnp.bfloat16


def horner(coefs, z):
    total = jnp.full_like(z, coefs[-1])
    for coef in coefs[-2::-1]:
        total = total * z + coef
    return total


def cos_sin(turns):
    part = turns - jnp.round(turns)
    square = part * part
    half_sin = part * horner(SIN, square)
    half_cos = horner(COS, square)
    return 1.0 - half_sin * half_sin, half_sin * half_cos


def one_less_exp(y, fade):
    series = y * horner((1.0, -1 / 2, 1 / 6, -1 / 24, 1 / 120, -1 / 720), y)
    return jnp.where(y < 0.4, series, 1.0 - fade * fade)


def cmul(a, b):
    return a[0] * b[0] - a[1] * b[1], a[0] * b[1] + a[1] * b[0]


def decay_of(rate, angle, time):
    fade = jnp.exp2(time * (rate * (-math.log2(math.e))))
    cosine, sine = cos_sin(time * (angle * (0.5 / math.pi)))
    return fade * cosine, fade * sine


def kernel(
    sp_size, tp_size,
    tokens_ref, elapsed_ref, norm_ref, drive_ref, read_ref, rate_ref, angle_ref,
    skip_ref, bias_ref, gain_ref, in_hbm, glu_hbm, out_hbm,
    mixed_ref,
    in_ref, glu_ref, out_ref, e_ref, driven_ref, proj_ref, sre, sim, pre, pim,
    ends, segs, st_ref, resp_ref,
    send1, recv1, send2, recv2, send3, recv3,
    wsem, s1s, r1s, s2s, r2s, s3s, r3s,
):
    rows = tokens_ref.shape[0]
    steps = rows // SUB
    pairs = rate_ref.shape[1]
    per = pairs // tp_size
    blocks = driven_ref.shape[1] // LANES
    inner = pairs // blocks
    wide = LANES // inner
    my_sp, my_tp = lax.axis_index("sp"), lax.axis_index("tp")

    loads = [
        pltpu.make_async_copy(a, b, wsem.at[i])
        for i, (a, b) in enumerate(((in_hbm, in_ref), (glu_hbm, glu_ref), (out_hbm, out_ref)))
    ]
    for load in loads:
        load.start()
    barrier = pltpu.get_barrier_semaphore()
    for off in range(1, tp_size):
        pl.semaphore_signal(
            barrier, inc=1, device_id=(my_sp, lax.rem(my_tp + off, tp_size)),
            device_id_type=pl.DeviceIdType.MESH,
        )
    for off in range(1, sp_size):
        pl.semaphore_signal(
            barrier, inc=1, device_id=(lax.rem(my_sp + off, sp_size), my_tp),
            device_id_type=pl.DeviceIdType.MESH,
        )

    at_row = lax.broadcasted_iota(jnp.int32, (rows, rows), 0)
    at_col = lax.broadcasted_iota(jnp.int32, (rows, rows), 1)
    place = at_col == (at_row & (SUB - 1)) * steps + (at_row >> 3)
    permute = place.astype(F32).astype(BF16)
    back = (at_row == (at_col & (SUB - 1)) * steps + (at_col >> 3)).astype(F32).astype(BF16)
    e_row = elapsed_ref[...]
    total_time = jnp.sum(e_row, axis=1, keepdims=True)
    e_ref[...] = jnp.broadcast_to(
        jnp.sum(jnp.where(place, e_row, 0.0), axis=1, keepdims=True), (rows, LANES)
    )

    values = tokens_ref[...].astype(F32)
    scale = lax.rsqrt(jnp.mean(values * values, axis=-1, keepdims=True) + epsilon)
    normed = (values * scale * norm_ref[...]).astype(BF16)
    loads[0].wait()
    driven = jnp.dot(normed, in_ref[...], preferred_element_type=F32).astype(BF16)
    driven_ref[...] = jnp.dot(permute, driven, preferred_element_type=F32).astype(BF16)

    lane = lax.broadcasted_iota(jnp.int32, (1, LANES), 1)

    def unit(k, r):
        rate = rate_ref[k, pl.ds(r, 1), :]
        twice = jnp.broadcast_to(rate * 2.0, (SUB, LANES))
        slope = jnp.broadcast_to(rate * (-math.log2(math.e)), (SUB, LANES))
        spin = jnp.broadcast_to(angle_ref[k, pl.ds(r, 1), :] * (0.5 / math.pi), (SUB, LANES))
        state = prod = None
        order = range(steps) if k == 0 else range(steps - 1, -1, -1)
        for j in order:
            at = slice(j * SUB, (j + 1) * SUB)
            e = e_ref[at, :]
            fade = jnp.exp2(e * slope)
            rise = one_less_exp(e * twice, fade)
            damping = rise * lax.rsqrt(jnp.maximum(rise, 1e-36))
            cosine, sine = cos_sin(e * spin)
            decay = (fade * cosine, fade * sine)
            push_re = proj_ref[at, k * 256 : k * 256 + 128] * damping
            push_im = proj_ref[at, k * 256 + 128 : k * 256 + 256] * damping
            if state is None:
                state, prod = (push_re, push_im), decay
            else:
                moved = cmul(decay, state)
                state = (moved[0] + push_re, moved[1] + push_im)
                prod = cmul(decay, prod)
            sre[k, r, at, :] = state[0]
            sim[k, r, at, :] = state[1]
            pre[k, r, at, :] = prod[0]
            pim[k, r, at, :] = prod[1]
        ends[k, 0, r] = state[0]
        ends[k, 1, r] = state[1]
        ends[k, 2, r] = prod[0]
        ends[k, 3, r] = prod[1]

    def block(b, carry):
        start = pl.multiple_of(b * LANES, LANES)
        piece = driven_ref[:, pl.ds(start, LANES)]
        weight = drive_ref[pl.ds(start, LANES), :]

        def one(i, carry):
            mask = (lane // wide == i).astype(F32).astype(BF16)
            proj_ref[...] = jnp.dot(piece * mask, weight, preferred_element_type=F32)
            unit(0, b * inner + i)
            unit(1, b * inner + i)
            return carry

        return lax.fori_loop(0, inner, one, carry)

    lax.fori_loop(0, blocks, block, 0)

    sub = lax.broadcasted_iota(jnp.int32, (per, SUB, LANES), 1)
    for q in range(tp_size):
        for k in range(2):
            at = slice(q * per, (q + 1) * per)
            s = (ends[k, 0, at], ends[k, 1, at])
            p = (ends[k, 2, at], ends[k, 3, at])

            def shift(x, far, fill):
                moved = pltpu.roll(x, far if k == 0 else SUB - far, 1)
                keep = sub >= far if k == 0 else sub < SUB - far
                return jnp.where(keep, moved, fill)

            for far in (1, 2, 4):
                old_s = (shift(s[0], far, 0.0), shift(s[1], far, 0.0))
                old_p = (shift(p[0], far, 1.0), shift(p[1], far, 0.0))
                moved = cmul(p, old_s)
                s = (moved[0] + s[0], moved[1] + s[1])
                p = cmul(p, old_p)
            last = SUB - 1 if k == 0 else 0
            send1[q, 2 * k] = s[0][:, last, :]
            send1[q, 2 * k + 1] = s[1][:, last, :]
            segs[k, 0, at] = shift(s[0], 1, 0.0)
            segs[k, 1, at] = shift(s[1], 1, 0.0)
            segs[k, 2, at] = shift(p[0], 1, 1.0)
            segs[k, 3, at] = shift(p[1], 1, 0.0)
        send1[q, 4] = jnp.broadcast_to(total_time, (per, LANES))

    pl.semaphore_wait(barrier, tp_size + sp_size - 2)

    def exchange_tp(send, recv, ssem, rsem):
        outs = []
        for off in range(1, tp_size):
            peer = lax.rem(my_tp + off, tp_size)
            copy = pltpu.make_async_remote_copy(
                src_ref=send.at[peer], dst_ref=recv.at[my_tp],
                send_sem=ssem.at[peer], recv_sem=rsem.at[my_tp],
                device_id=(my_sp, peer), device_id_type=pl.DeviceIdType.MESH,
            )
            copy.start()
            outs.append(copy)
        recv[my_tp] = send[my_tp]
        for off in range(1, tp_size):
            peer = lax.rem(my_tp + off, tp_size)
            pltpu.make_async_remote_copy(
                src_ref=send.at[peer], dst_ref=recv.at[peer],
                send_sem=ssem.at[peer], recv_sem=rsem.at[peer],
                device_id=(my_sp, peer), device_id_type=pl.DeviceIdType.MESH,
            ).wait_recv()
        return outs

    pending = exchange_tp(send1, recv1, s1s, r1s)
    mine = pl.ds(my_tp * per, per)
    rate = (rate_ref[0, mine, :], rate_ref[1, mine, :])
    angle = (angle_ref[0, mine, :], angle_ref[1, mine, :])
    fold = []
    for k in range(2):
        fold.append([decay_of(rate[k], angle[k], recv1[i, 4]) for i in range(tp_size)])
    group_time = recv1[0, 4]
    for i in range(1, tp_size):
        group_time = group_time + recv1[i, 4]
    for k in range(2):
        total = None
        for i in range(tp_size) if k == 0 else range(tp_size - 1, -1, -1):
            s = (recv1[i, 2 * k], recv1[i, 2 * k + 1])
            if total is None:
                total = s
            else:
                moved = cmul(fold[k][i], total)
                total = (moved[0] + s[0], moved[1] + s[1])
        send2[2 * k] = total[0]
        send2[2 * k + 1] = total[1]
    send2[4] = group_time

    for off in range(1, sp_size):
        peer = lax.rem(my_sp + off, sp_size)
        copy = pltpu.make_async_remote_copy(
            src_ref=send2, dst_ref=recv2.at[my_sp],
            send_sem=s2s.at[peer], recv_sem=r2s.at[my_sp],
            device_id=(peer, my_tp), device_id_type=pl.DeviceIdType.MESH,
        )
        copy.start()
        pending.append(copy)
    recv2[my_sp] = send2[...]
    for off in range(1, sp_size):
        peer = lax.rem(my_sp + off, sp_size)
        pltpu.make_async_remote_copy(
            src_ref=send2, dst_ref=recv2.at[peer],
            send_sem=s2s.at[peer], recv_sem=r2s.at[peer],
            device_id=(peer, my_tp), device_id_type=pl.DeviceIdType.MESH,
        ).wait_recv()

    for k in range(2):
        enter = (jnp.zeros((per, LANES), F32), jnp.zeros((per, LANES), F32))
        for i in range(sp_size) if k == 0 else range(sp_size - 1, -1, -1):
            moved = cmul(decay_of(rate[k], angle[k], recv2[i, 4]), enter)
            reached = (jnp.full((per, LANES), i, jnp.int32) < my_sp) if k == 0 else (
                jnp.full((per, LANES), i, jnp.int32) > my_sp
            )
            enter = tuple(
                jnp.where(reached, moved[c] + recv2[i, 2 * k + c], enter[c]) for c in range(2)
            )
        for i in range(tp_size) if k == 0 else range(tp_size - 1, -1, -1):
            send3[i, 2 * k] = enter[0]
            send3[i, 2 * k + 1] = enter[1]
            moved = cmul(fold[k][i], enter)
            enter = tuple(moved[c] + recv1[i, 2 * k + c] for c in range(2))
    pending = pending + exchange_tp(send3, recv3, s3s, r3s)

    def read_block(b, carry):
        start = pl.multiple_of(b * LANES, LANES)
        weight = read_ref[pl.ds(start, LANES), :]

        def one(i, total):
            r = b * inner + i
            q, row = r // per, lax.rem(r, per)
            for k in range(2):
                enter = (
                    recv3[q, 2 * k, pl.ds(row, 1), :],
                    recv3[q, 2 * k + 1, pl.ds(row, 1), :],
                )
                moved = cmul((segs[k, 2, r], segs[k, 3, r]), enter)
                enter = (moved[0] + segs[k, 0, r], moved[1] + segs[k, 1, r])
                shape = (steps, SUB, LANES)
                prod = (pre[k, r].reshape(shape), pim[k, r].reshape(shape))
                moved = cmul(prod, enter)
                whole_re = sre[k, r].reshape(shape) + moved[0]
                whole_im = sim[k, r].reshape(shape) + moved[1]
                st_ref[:, k * 256 : k * 256 + 128] = whole_re.reshape(rows, LANES).astype(BF16)
                st_ref[:, k * 256 + 128 : k * 256 + 256] = whole_im.reshape(rows, LANES).astype(BF16)
            out = lax.dot_general(
                st_ref[...], weight, (((1,), (1,)), ((), ())), preferred_element_type=F32
            )
            return jnp.where(lane // wide == i, out, total)

        resp_ref[:, pl.ds(start, LANES)] = lax.fori_loop(
            0, inner, one, jnp.zeros((rows, LANES), F32)
        )
        return carry

    lax.fori_loop(0, blocks, read_block, 0)

    response = resp_ref[...] + skip_ref[...] * driven_ref[...].astype(F32)
    active = jax.nn.gelu(response)
    loads[1].wait()
    gate = jnp.dot(active.astype(BF16), glu_ref[...], preferred_element_type=F32) + bias_ref[...]
    gated = (active * jax.nn.sigmoid(gate)).astype(BF16)
    gated = jnp.dot(back, gated, preferred_element_type=F32).astype(BF16)
    loads[2].wait()
    projected = jnp.dot(gated, out_ref[...], preferred_element_type=F32)
    scale = lax.rsqrt(jnp.mean(projected * projected, axis=-1, keepdims=True) + epsilon)
    mixed_ref[...] = (projected * scale * gain_ref[...]).astype(BF16)
    for copy in pending:
        copy.wait_send()


def local(
    sp_size, tp_size, tokens, elapsed, norm_gain, in_weight, state_input, state_output,
    forget_rate, decay_angle, skip_gain, glu_weight, glu_bias, out_weight, out_gain,
):
    rows, width = tokens.shape
    channels = in_weight.shape[1]
    _, _, groups, states, _ = state_input.shape
    share = LANES // states
    pairs = groups // share
    per = pairs // tp_size
    parity = (jnp.arange(groups)[:, None] % share == jnp.arange(share)[None, :])
    parity = parity[:, None, None, None, :, None]

    def spread(values):
        return jnp.where(parity, values[:, :, :, :, None, :], 0).astype(BF16).reshape(
            channels, 4 * LANES
        )

    drive = spread(state_input.transpose(2, 4, 0, 1, 3))
    sign = jnp.array([1.0, -1.0], F32)[None, :, None, None, None]
    read = spread((state_output * sign).transpose(2, 3, 0, 1, 4))

    vmem = pl.BlockSpec(memory_space=pltpu.VMEM)
    hbm = pl.BlockSpec(memory_space=pl.ANY)
    cells = (2, pairs, rows, LANES)
    dma = pltpu.SemaphoreType.DMA
    return pl.pallas_call(
        functools.partial(kernel, sp_size, tp_size),
        out_shape=jax.ShapeDtypeStruct((rows, width), BF16),
        in_specs=[vmem] * 10 + [hbm] * 3,
        out_specs=vmem,
        scratch_shapes=[
            pltpu.VMEM(in_weight.shape, BF16),
            pltpu.VMEM(glu_weight.shape, BF16),
            pltpu.VMEM(out_weight.shape, BF16),
            pltpu.VMEM((rows, LANES), F32),
            pltpu.VMEM((rows, channels), BF16),
            pltpu.VMEM((rows, 4 * LANES), F32),
            pltpu.VMEM(cells, F32),
            pltpu.VMEM(cells, F32),
            pltpu.VMEM(cells, F32),
            pltpu.VMEM(cells, F32),
            pltpu.VMEM((2, 4, pairs, SUB, LANES), F32),
            pltpu.VMEM((2, 4, pairs, SUB, LANES), F32),
            pltpu.VMEM((rows, 4 * LANES), BF16),
            pltpu.VMEM((rows, channels), F32),
            pltpu.VMEM((tp_size, 5, per, LANES), F32),
            pltpu.VMEM((tp_size, 5, per, LANES), F32),
            pltpu.VMEM((5, per, LANES), F32),
            pltpu.VMEM((sp_size, 5, per, LANES), F32),
            pltpu.VMEM((tp_size, 4, per, LANES), F32),
            pltpu.VMEM((tp_size, 4, per, LANES), F32),
            dma((3,)),
            dma((tp_size,)),
            dma((tp_size,)),
            dma((sp_size,)),
            dma((sp_size,)),
            dma((tp_size,)),
            dma((tp_size,)),
        ],
        compiler_params=pltpu.CompilerParams(
            collective_id=0, has_side_effects=True, vmem_limit_bytes=60 * 1024 * 1024
        ),
    )(
        tokens, elapsed.reshape(1, rows), norm_gain.reshape(1, -1), drive, read,
        forget_rate.reshape(2, pairs, LANES), decay_angle.reshape(2, pairs, LANES),
        skip_gain.reshape(1, -1), glu_bias.reshape(1, -1), out_gain.reshape(1, -1),
        in_weight, glu_weight, out_weight,
    )


def solution(mesh):
    rows = P(("sp", "tp"), None)
    return jax.shard_map(
        functools.partial(local, mesh.shape["sp"], mesh.shape["tp"]),
        mesh=mesh,
        in_specs=(rows, P(("sp", "tp"))) + (P(),) * 11,
        out_specs=rows,
        check_vma=False,
    )
```

```python
import functools
import math

import jax
import jax.numpy as jnp
import numpy as np
from jax import lax
from jax.experimental import pallas as pl
from jax.experimental.pallas import tpu as pltpu
from jax.sharding import PartitionSpec as P

epsilon = 1e-06
LANES = 128
NODES = 16
SPAN = 3.0
SUB = 8
SIN = (4.44288292, -7.30824569, 3.60635422, -0.84611165, 0.10982452)
COS = (1.41421356, -6.97886411, 5.73988154, -1.88827492, 0.33225154, -0.03450161)
F32 = jnp.float32
BF16 = jnp.bfloat16


def horner(coefs, z):
    total = jnp.full_like(z, coefs[-1])
    for coef in coefs[-2::-1]:
        total = total * z + coef
    return total


def cos_sin(turns):
    part = turns - jnp.round(turns)
    square = part * part
    half_sin = part * horner(SIN, square)
    half_cos = horner(COS, square)
    return 1.0 - half_sin * half_sin, half_sin * half_cos


def one_less_exp(y, fade):
    series = y * horner((1.0, -1 / 2, 1 / 6, -1 / 24, 1 / 120, -1 / 720), y)
    return jnp.where(y < 0.4, series, 1.0 - fade * fade)


def cmul(a, b):
    return a[0] * b[0] - a[1] * b[1], a[0] * b[1] + a[1] * b[0]


def decay_of(rate, angle, time):
    fade = jnp.exp2(time * (rate * (-math.log2(math.e))))
    cosine, sine = cos_sin(time * (angle * (0.5 / math.pi)))
    return fade * cosine, fade * sine


def kernel(
    sp_size, tp_size,
    tokens_ref, elapsed_ref, norm_ref, rate_raw, angle_raw, skip_ref, bias_ref, gain_ref,
    basis_ref, node_ref, drive_hbm, in_hbm, read_hbm, glu_hbm, out_hbm,
    mixed_ref,
    drive_raw, in_ref, read_raw, glu_ref, out_ref, rate_ref, angle_ref, drive_ref, read_ref,
    rhs_ref, dec_ref, driven_ref, proj_ref, sre, sim, pre, pim,
    ends, segs, st_ref, resp_ref,
    send1, recv1, send2, recv2, send3, recv3,
    wsem, s1s, r1s, s2s, r2s, s3s, r3s,
):
    rows = tokens_ref.shape[0]
    steps = rows // SUB
    pairs = rate_ref.shape[1]
    states = rate_raw.shape[2]
    share = LANES // states
    group_width = driven_ref.shape[1] // rate_raw.shape[1]
    per = pairs // tp_size
    blocks = driven_ref.shape[1] // LANES
    inner = pairs // blocks
    wide = LANES // inner
    my_sp, my_tp = lax.axis_index("sp"), lax.axis_index("tp")

    loads = [
        pltpu.make_async_copy(a, b, wsem.at[i])
        for i, (a, b) in enumerate((
            (drive_hbm, drive_raw), (in_hbm, in_ref), (read_hbm, read_raw),
            (glu_hbm, glu_ref), (out_hbm, out_ref),
        ))
    ]
    for load in loads:
        load.start()
    barrier = pltpu.get_barrier_semaphore()
    for off in range(1, tp_size):
        pl.semaphore_signal(
            barrier, inc=1, device_id=(my_sp, lax.rem(my_tp + off, tp_size)),
            device_id_type=pl.DeviceIdType.MESH,
        )
    for off in range(1, sp_size):
        pl.semaphore_signal(
            barrier, inc=1, device_id=(lax.rem(my_sp + off, sp_size), my_tp),
            device_id_type=pl.DeviceIdType.MESH,
        )

    at_row = lax.broadcasted_iota(jnp.int32, (rows, rows), 0)
    at_col = lax.broadcasted_iota(jnp.int32, (rows, rows), 1)
    place = at_col == (at_row & (SUB - 1)) * steps + (at_row >> 3)
    permute = place.astype(F32).astype(BF16)
    back = (at_row == (at_col & (SUB - 1)) * steps + (at_col >> 3)).astype(F32).astype(BF16)
    e_row = elapsed_ref[...]
    total_time = jnp.sum(e_row, axis=1, keepdims=True)
    e_col = jnp.broadcast_to(
        jnp.sum(jnp.where(place, e_row, 0.0), axis=1, keepdims=True), (rows, LANES)
    )
    x = e_col * (2.0 / SPAN) - 1.0
    older, newer = jnp.ones_like(x), x
    lagrange = basis_ref[0:1, :] + basis_ref[1:2, :] * x
    for n in range(2, NODES):
        older, newer = newer, 2.0 * x * newer - older
        lagrange = lagrange + basis_ref[n : n + 1, :] * newer
    part = lax.broadcasted_iota(jnp.int32, (rows, LANES), 1) // NODES

    def split(values):
        high = values.astype(BF16).astype(F32)
        rest = values - high
        middle = rest.astype(BF16).astype(F32)
        return high, middle, rest - middle

    def factor(values):
        high, middle, low = split(values)
        picked = jnp.where(part < 3, high, jnp.where(part < 5, middle, low))
        return jnp.where(part < 6, picked, 0.0).astype(BF16)

    basis = factor(lagrange)
    rooted = factor(lagrange * jnp.sqrt(e_col))
    for k in range(2):
        for raw, packed in ((rate_raw, rate_ref), (angle_raw, angle_ref)):
            packed[k] = jnp.concatenate(
                [raw[k, pl.ds(m, pairs, stride=share), :] for m in range(share)], axis=1
            )
    owner = lax.broadcasted_iota(jnp.int32, (LANES, states), 0) // group_width % share

    def spread(raw, target, start, at_row, negate):
        for k in range(2):
            for c in range(2):
                piece = raw[k, c, pl.ds(start, LANES), :].astype(F32)
                if negate and c == 1:
                    piece = -piece
                target[pl.ds(at_row, LANES), (2 * k + c) * LANES : (2 * k + c + 1) * LANES] = (
                    jnp.concatenate(
                        [jnp.where(owner == m, piece, 0.0) for m in range(share)], axis=1
                    ).astype(BF16)
                )

    values = tokens_ref[...].astype(F32)
    scale = lax.rsqrt(jnp.mean(values * values, axis=-1, keepdims=True) + epsilon)
    normed = (values * scale * norm_ref[...]).astype(BF16)
    loads[1].wait()
    driven = jnp.dot(normed, in_ref[...], preferred_element_type=F32).astype(BF16)
    driven_ref[...] = jnp.dot(permute, driven, preferred_element_type=F32).astype(BF16)

    lane = lax.broadcasted_iota(jnp.int32, (1, LANES), 1)

    nodes = node_ref[...]

    def tabulate(k, r):
        rate = rate_ref[k, pl.ds(r, 1), :]
        angle = angle_ref[k, pl.ds(r, 1), :]
        y = nodes * (rate * 2.0)
        fade = jnp.exp2(nodes * (rate * (-math.log2(math.e))))
        rise = one_less_exp(y, fade) / nodes
        root = rise * lax.rsqrt(jnp.maximum(rise, 1e-36))
        cosine, sine = cos_sin(nodes * (angle * (0.5 / math.pi)))
        for at, values in ((2 * k, fade * cosine), (2 * k + 1, fade * sine), (4 + k, root)):
            parts = split(values)
            for n, which in enumerate((0, 1, 2, 0, 1, 0, 0, 0)):
                rhs_ref[n * NODES : (n + 1) * NODES, at * LANES : (at + 1) * LANES] = (
                    parts[which].astype(BF16)
                )

    def unit(k, r):
        state = prod = None
        order = range(steps) if k == 0 else range(steps - 1, -1, -1)
        for j in order:
            at = slice(j * SUB, (j + 1) * SUB)
            decay = (
                dec_ref[at, k * 256 : k * 256 + 128], dec_ref[at, k * 256 + 128 : k * 256 + 256]
            )
            damping = dec_ref[at, 512 + k * 128 : 640 + k * 128]
            push_re = proj_ref[at, k * 256 : k * 256 + 128] * damping
            push_im = proj_ref[at, k * 256 + 128 : k * 256 + 256] * damping
            if state is None:
                state, prod = (push_re, push_im), decay
            else:
                moved = cmul(decay, state)
                state = (moved[0] + push_re, moved[1] + push_im)
                prod = cmul(decay, prod)
            sre[k, r, at, :] = state[0]
            sim[k, r, at, :] = state[1]
            pre[k, r, at, :] = prod[0]
            pim[k, r, at, :] = prod[1]
        ends[k, 0, r] = state[0]
        ends[k, 1, r] = state[1]
        ends[k, 2, r] = prod[0]
        ends[k, 3, r] = prod[1]

    def block(b, carry):
        start = pl.multiple_of(b * LANES, LANES)
        piece = driven_ref[:, pl.ds(start, LANES)]
        spread(drive_raw, drive_ref, start, 0, False)
        weight = drive_ref[...]

        def one(i, carry):
            mask = (lane // wide == i).astype(F32).astype(BF16)
            proj_ref[...] = jnp.dot(piece * mask, weight, preferred_element_type=F32)
            tabulate(0, b * inner + i)
            tabulate(1, b * inner + i)
            dec_ref[:, :512] = jnp.dot(basis, rhs_ref[:, :512], preferred_element_type=F32)
            dec_ref[:, 512:] = jnp.dot(rooted, rhs_ref[:, 512:], preferred_element_type=F32)
            unit(0, b * inner + i)
            unit(1, b * inner + i)
            return carry

        return lax.fori_loop(0, inner, one, carry)

    loads[0].wait()
    lax.fori_loop(0, blocks, block, 0)

    sub = lax.broadcasted_iota(jnp.int32, (per, SUB, LANES), 1)
    for q in range(tp_size):
        for k in range(2):
            at = slice(q * per, (q + 1) * per)
            s = (ends[k, 0, at], ends[k, 1, at])
            p = (ends[k, 2, at], ends[k, 3, at])

            def shift(x, far, fill):
                moved = pltpu.roll(x, far if k == 0 else SUB - far, 1)
                keep = sub >= far if k == 0 else sub < SUB - far
                return jnp.where(keep, moved, fill)

            for far in (1, 2, 4):
                old_s = (shift(s[0], far, 0.0), shift(s[1], far, 0.0))
                old_p = (shift(p[0], far, 1.0), shift(p[1], far, 0.0))
                moved = cmul(p, old_s)
                s = (moved[0] + s[0], moved[1] + s[1])
                p = cmul(p, old_p)
            last = SUB - 1 if k == 0 else 0
            send1[q, 2 * k] = s[0][:, last, :]
            send1[q, 2 * k + 1] = s[1][:, last, :]
            segs[k, 0, at] = shift(s[0], 1, 0.0)
            segs[k, 1, at] = shift(s[1], 1, 0.0)
            segs[k, 2, at] = shift(p[0], 1, 1.0)
            segs[k, 3, at] = shift(p[1], 1, 0.0)
        send1[q, 4] = jnp.broadcast_to(total_time, (per, LANES))

    pl.semaphore_wait(barrier, tp_size + sp_size - 2)

    def exchange_tp(send, recv, ssem, rsem, meanwhile=None):
        outs = []
        for off in range(1, tp_size):
            peer = lax.rem(my_tp + off, tp_size)
            copy = pltpu.make_async_remote_copy(
                src_ref=send.at[peer], dst_ref=recv.at[my_tp],
                send_sem=ssem.at[peer], recv_sem=rsem.at[my_tp],
                device_id=(my_sp, peer), device_id_type=pl.DeviceIdType.MESH,
            )
            copy.start()
            outs.append(copy)
        recv[my_tp] = send[my_tp]
        if meanwhile is not None:
            meanwhile()
        for off in range(1, tp_size):
            peer = lax.rem(my_tp + off, tp_size)
            pltpu.make_async_remote_copy(
                src_ref=send.at[peer], dst_ref=recv.at[peer],
                send_sem=ssem.at[peer], recv_sem=rsem.at[peer],
                device_id=(my_sp, peer), device_id_type=pl.DeviceIdType.MESH,
            ).wait_recv()
        return outs

    def prepare_read():
        loads[2].wait()

        def piece(b, carry):
            start = pl.multiple_of(b * LANES, LANES)
            spread(read_raw, read_ref, start, start, True)
            return carry

        lax.fori_loop(0, blocks, piece, 0)

    pending = exchange_tp(send1, recv1, s1s, r1s, prepare_read)
    mine = pl.ds(my_tp * per, per)
    rate = (rate_ref[0, mine, :], rate_ref[1, mine, :])
    angle = (angle_ref[0, mine, :], angle_ref[1, mine, :])
    fold = []
    for k in range(2):
        fold.append([decay_of(rate[k], angle[k], recv1[i, 4]) for i in range(tp_size)])
    group_time = recv1[0, 4]
    for i in range(1, tp_size):
        group_time = group_time + recv1[i, 4]
    for k in range(2):
        total = None
        for i in range(tp_size) if k == 0 else range(tp_size - 1, -1, -1):
            s = (recv1[i, 2 * k], recv1[i, 2 * k + 1])
            if total is None:
                total = s
            else:
                moved = cmul(fold[k][i], total)
                total = (moved[0] + s[0], moved[1] + s[1])
        send2[2 * k] = total[0]
        send2[2 * k + 1] = total[1]
    send2[4] = group_time

    for off in range(1, sp_size):
        peer = lax.rem(my_sp + off, sp_size)
        copy = pltpu.make_async_remote_copy(
            src_ref=send2, dst_ref=recv2.at[my_sp],
            send_sem=s2s.at[peer], recv_sem=r2s.at[my_sp],
            device_id=(peer, my_tp), device_id_type=pl.DeviceIdType.MESH,
        )
        copy.start()
        pending.append(copy)
    recv2[my_sp] = send2[...]
    for off in range(1, sp_size):
        peer = lax.rem(my_sp + off, sp_size)
        pltpu.make_async_remote_copy(
            src_ref=send2, dst_ref=recv2.at[peer],
            send_sem=s2s.at[peer], recv_sem=r2s.at[peer],
            device_id=(peer, my_tp), device_id_type=pl.DeviceIdType.MESH,
        ).wait_recv()

    for k in range(2):
        enter = (jnp.zeros((per, LANES), F32), jnp.zeros((per, LANES), F32))
        for i in range(sp_size) if k == 0 else range(sp_size - 1, -1, -1):
            moved = cmul(decay_of(rate[k], angle[k], recv2[i, 4]), enter)
            reached = (jnp.full((per, LANES), i, jnp.int32) < my_sp) if k == 0 else (
                jnp.full((per, LANES), i, jnp.int32) > my_sp
            )
            enter = tuple(
                jnp.where(reached, moved[c] + recv2[i, 2 * k + c], enter[c]) for c in range(2)
            )
        for i in range(tp_size) if k == 0 else range(tp_size - 1, -1, -1):
            send3[i, 2 * k] = enter[0]
            send3[i, 2 * k + 1] = enter[1]
            moved = cmul(fold[k][i], enter)
            enter = tuple(moved[c] + recv1[i, 2 * k + c] for c in range(2))
    pending = pending + exchange_tp(send3, recv3, s3s, r3s)

    def read_block(b, carry):
        start = pl.multiple_of(b * LANES, LANES)
        weight = read_ref[pl.ds(start, LANES), :]

        def one(i, total):
            r = b * inner + i
            q, row = r // per, lax.rem(r, per)
            for k in range(2):
                enter = (
                    recv3[q, 2 * k, pl.ds(row, 1), :],
                    recv3[q, 2 * k + 1, pl.ds(row, 1), :],
                )
                moved = cmul((segs[k, 2, r], segs[k, 3, r]), enter)
                enter = (moved[0] + segs[k, 0, r], moved[1] + segs[k, 1, r])
                shape = (steps, SUB, LANES)
                prod = (pre[k, r].reshape(shape), pim[k, r].reshape(shape))
                moved = cmul(prod, enter)
                whole_re = sre[k, r].reshape(shape) + moved[0]
                whole_im = sim[k, r].reshape(shape) + moved[1]
                st_ref[:, k * 256 : k * 256 + 128] = whole_re.reshape(rows, LANES).astype(BF16)
                st_ref[:, k * 256 + 128 : k * 256 + 256] = whole_im.reshape(rows, LANES).astype(BF16)
            out = lax.dot_general(
                st_ref[...], weight, (((1,), (1,)), ((), ())), preferred_element_type=F32
            )
            return jnp.where(lane // wide == i, out, total)

        resp_ref[:, pl.ds(start, LANES)] = lax.fori_loop(
            0, inner, one, jnp.zeros((rows, LANES), F32)
        )
        return carry

    lax.fori_loop(0, blocks, read_block, 0)

    response = resp_ref[...] + skip_ref[...] * driven_ref[...].astype(F32)
    active = jax.nn.gelu(response)
    loads[3].wait()
    gate = jnp.dot(active.astype(BF16), glu_ref[...], preferred_element_type=F32) + bias_ref[...]
    gated = (active * jax.nn.sigmoid(gate)).astype(BF16)
    gated = jnp.dot(back, gated, preferred_element_type=F32).astype(BF16)
    loads[4].wait()
    projected = jnp.dot(gated, out_ref[...], preferred_element_type=F32)
    scale = lax.rsqrt(jnp.mean(projected * projected, axis=-1, keepdims=True) + epsilon)
    mixed_ref[...] = (projected * scale * gain_ref[...]).astype(BF16)
    for copy in pending:
        copy.wait_send()


def local(
    sp_size, tp_size, tokens, elapsed, norm_gain, in_weight, state_input, state_output,
    forget_rate, decay_angle, skip_gain, glu_weight, glu_bias, out_weight, out_gain,
):
    rows, width = tokens.shape
    channels = in_weight.shape[1]
    _, _, groups, states, _ = state_input.shape
    share = LANES // states
    pairs = groups // share
    per = pairs // tp_size
    drive = state_input.transpose(0, 1, 2, 4, 3).reshape(2, 2, channels, states)
    read = state_output.reshape(2, 2, channels, states)
    turns = np.pi * (np.arange(LANES) % NODES + 0.5) / NODES
    orders = np.arange(NODES)[:, None]
    basis = np.cos(orders * turns[None, :]) * np.where(orders == 0, 1, 2) / NODES
    nodes = np.broadcast_to((np.cos(turns[:NODES, None]) + 1) * (SPAN / 2), (NODES, LANES))

    vmem = pl.BlockSpec(memory_space=pltpu.VMEM)
    hbm = pl.BlockSpec(memory_space=pl.ANY)
    cells = (2, pairs, rows, LANES)
    dma = pltpu.SemaphoreType.DMA
    return pl.pallas_call(
        functools.partial(kernel, sp_size, tp_size),
        out_shape=jax.ShapeDtypeStruct((rows, width), BF16),
        in_specs=[vmem] * 10 + [hbm] * 5,
        out_specs=vmem,
        scratch_shapes=[
            pltpu.VMEM(drive.shape, BF16),
            pltpu.VMEM(in_weight.shape, BF16),
            pltpu.VMEM(read.shape, F32),
            pltpu.VMEM(glu_weight.shape, BF16),
            pltpu.VMEM(out_weight.shape, BF16),
            pltpu.VMEM((2, pairs, LANES), F32),
            pltpu.VMEM((2, pairs, LANES), F32),
            pltpu.VMEM((LANES, 4 * LANES), BF16),
            pltpu.VMEM((channels, 4 * LANES), BF16),
            pltpu.VMEM((LANES, 6 * LANES), BF16),
            pltpu.VMEM((rows, 6 * LANES), F32),
            pltpu.VMEM((rows, channels), BF16),
            pltpu.VMEM((rows, 4 * LANES), F32),
            pltpu.VMEM(cells, F32),
            pltpu.VMEM(cells, F32),
            pltpu.VMEM(cells, F32),
            pltpu.VMEM(cells, F32),
            pltpu.VMEM((2, 4, pairs, SUB, LANES), F32),
            pltpu.VMEM((2, 4, pairs, SUB, LANES), F32),
            pltpu.VMEM((rows, 4 * LANES), BF16),
            pltpu.VMEM((rows, channels), F32),
            pltpu.VMEM((tp_size, 5, per, LANES), F32),
            pltpu.VMEM((tp_size, 5, per, LANES), F32),
            pltpu.VMEM((5, per, LANES), F32),
            pltpu.VMEM((sp_size, 5, per, LANES), F32),
            pltpu.VMEM((tp_size, 4, per, LANES), F32),
            pltpu.VMEM((tp_size, 4, per, LANES), F32),
            dma((5,)),
            dma((tp_size,)),
            dma((tp_size,)),
            dma((sp_size,)),
            dma((sp_size,)),
            dma((tp_size,)),
            dma((tp_size,)),
        ],
        compiler_params=pltpu.CompilerParams(
            collective_id=0, has_side_effects=True, vmem_limit_bytes=60 * 1024 * 1024
        ),
    )(
        tokens, elapsed.reshape(1, rows), norm_gain.reshape(1, -1), forget_rate, decay_angle,
        skip_gain.reshape(1, -1), glu_bias.reshape(1, -1), out_gain.reshape(1, -1),
        jnp.asarray(basis, F32), jnp.asarray(nodes, F32),
        drive, in_weight, read, glu_weight, out_weight,
    )


def solution(mesh):
    rows = P(("sp", "tp"), None)
    return jax.shard_map(
        functools.partial(local, mesh.shape["sp"], mesh.shape["tp"]),
        mesh=mesh,
        in_specs=(rows, P(("sp", "tp"))) + (P(),) * 11,
        out_specs=rows,
        check_vma=False,
    )
```

```python
import functools
import math

import jax
import jax.numpy as jnp
import numpy as np
from jax import lax
from jax.experimental import pallas as pl
from jax.experimental.pallas import tpu as pltpu
from jax.sharding import PartitionSpec as P

epsilon = 1e-06
LANES = 128
NODES = 16
SPAN = 3.0
SUB = 8
SIN = (4.44288292, -7.30824569, 3.60635422, -0.84611165, 0.10982452)
COS = (1.41421356, -6.97886411, 5.73988154, -1.88827492, 0.33225154, -0.03450161)
F32 = jnp.float32
BF16 = jnp.bfloat16


def horner(coefs, z):
    total = jnp.full_like(z, coefs[-1])
    for coef in coefs[-2::-1]:
        total = total * z + coef
    return total


def cos_sin(turns):
    part = turns - jnp.round(turns)
    square = part * part
    half_sin = part * horner(SIN, square)
    half_cos = horner(COS, square)
    return 1.0 - half_sin * half_sin, half_sin * half_cos


def one_less_exp(y, fade):
    series = y * horner((1.0, -1 / 2, 1 / 6, -1 / 24, 1 / 120, -1 / 720), y)
    return jnp.where(y < 0.4, series, 1.0 - fade * fade)


def cmul(a, b):
    return a[0] * b[0] - a[1] * b[1], a[0] * b[1] + a[1] * b[0]


def decay_of(rate, angle, time):
    fade = jnp.exp2(time * (rate * (-math.log2(math.e))))
    cosine, sine = cos_sin(time * (angle * (0.5 / math.pi)))
    return fade * cosine, fade * sine


def kernel(
    sp_size, tp_size,
    tokens_ref, elapsed_ref, norm_ref, rate_raw, angle_raw, skip_ref, bias_ref, gain_ref,
    basis_ref, node_ref, drive_hbm, in_hbm, read_hbm, glu_hbm, out_hbm,
    mixed_ref,
    drive_raw, in_ref, read_raw, glu_ref, out_ref, rate_ref, angle_ref, drive_ref, read_ref,
    rhs_ref, dec_ref, driven_ref, proj_ref, sre, sim, pre, pim,
    ends, segs, st_ref, resp_ref,
    send1, recv1, send2, recv2, send3, recv3,
    wsem, s1s, r1s, s2s, r2s, s3s, r3s,
):
    rows = tokens_ref.shape[0]
    steps = rows // SUB
    pairs = rate_ref.shape[1]
    states = rate_raw.shape[2]
    share = LANES // states
    group_width = driven_ref.shape[1] // rate_raw.shape[1]
    per = pairs // tp_size
    blocks = driven_ref.shape[1] // LANES
    inner = pairs // blocks
    wide = LANES // inner
    my_sp, my_tp = lax.axis_index("sp"), lax.axis_index("tp")

    loads = [
        pltpu.make_async_copy(a, b, wsem.at[i])
        for i, (a, b) in enumerate((
            (drive_hbm, drive_raw), (in_hbm, in_ref), (read_hbm, read_raw),
            (glu_hbm, glu_ref), (out_hbm, out_ref),
        ))
    ]
    for load in loads[:2]:
        load.start()
    barrier = pltpu.get_barrier_semaphore()
    for off in range(1, tp_size):
        pl.semaphore_signal(
            barrier, inc=1, device_id=(my_sp, lax.rem(my_tp + off, tp_size)),
            device_id_type=pl.DeviceIdType.MESH,
        )
    for off in range(1, sp_size):
        pl.semaphore_signal(
            barrier, inc=1, device_id=(lax.rem(my_sp + off, sp_size), my_tp),
            device_id_type=pl.DeviceIdType.MESH,
        )

    at_row = lax.broadcasted_iota(jnp.int32, (rows, rows), 0)
    at_col = lax.broadcasted_iota(jnp.int32, (rows, rows), 1)
    place = at_col == (at_row & (SUB - 1)) * steps + (at_row >> 3)
    permute = place.astype(F32).astype(BF16)
    back = (at_row == (at_col & (SUB - 1)) * steps + (at_col >> 3)).astype(F32).astype(BF16)
    e_row = elapsed_ref[...]
    total_time = jnp.sum(e_row, axis=1, keepdims=True)
    e_col = jnp.broadcast_to(
        jnp.sum(jnp.where(place, e_row, 0.0), axis=1, keepdims=True), (rows, LANES)
    )
    x = e_col * (2.0 / SPAN) - 1.0
    older, newer = jnp.ones_like(x), x
    lagrange = basis_ref[0:1, :] + basis_ref[1:2, :] * x
    for n in range(2, NODES):
        older, newer = newer, 2.0 * x * newer - older
        lagrange = lagrange + basis_ref[n : n + 1, :] * newer
    part = lax.broadcasted_iota(jnp.int32, (rows, LANES), 1) // NODES

    def split(values):
        high = values.astype(BF16).astype(F32)
        rest = values - high
        middle = rest.astype(BF16).astype(F32)
        return high, middle, rest - middle

    def factor(values):
        high, middle, low = split(values)
        picked = jnp.where(part < 3, high, jnp.where(part < 5, middle, low))
        return jnp.where(part < 6, picked, 0.0).astype(BF16)

    basis = factor(lagrange)
    rooted = factor(lagrange * jnp.sqrt(e_col))
    for k in range(2):
        for raw, packed in ((rate_raw, rate_ref), (angle_raw, angle_ref)):
            packed[k] = jnp.concatenate(
                [raw[k, pl.ds(m, pairs, stride=share), :] for m in range(share)], axis=1
            )
    owner = lax.broadcasted_iota(jnp.int32, (LANES, states), 0) // group_width % share

    def spread(raw, target, start, at_row, negate):
        for k in range(2):
            for c in range(2):
                piece = raw[k, c, pl.ds(start, LANES), :].astype(F32)
                if negate and c == 1:
                    piece = -piece
                target[pl.ds(at_row, LANES), (2 * k + c) * LANES : (2 * k + c + 1) * LANES] = (
                    jnp.concatenate(
                        [jnp.where(owner == m, piece, 0.0) for m in range(share)], axis=1
                    ).astype(BF16)
                )

    nodes = node_ref[...]

    def tabulate(k, r):
        rate = rate_ref[k, pl.ds(r, 1), :]
        angle = angle_ref[k, pl.ds(r, 1), :]
        y = nodes * (rate * 2.0)
        fade = jnp.exp2(nodes * (rate * (-math.log2(math.e))))
        rise = one_less_exp(y, fade) / nodes
        root = rise * lax.rsqrt(jnp.maximum(rise, 1e-36))
        cosine, sine = cos_sin(nodes * (angle * (0.5 / math.pi)))
        for at, values in ((2 * k, fade * cosine), (2 * k + 1, fade * sine), (4 + k, root)):
            parts = split(values)
            for n, which in enumerate((0, 1, 2, 0, 1, 0, 0, 0)):
                rhs_ref[r, n * NODES : (n + 1) * NODES, at * LANES : (at + 1) * LANES] = (
                    parts[which].astype(BF16)
                )

    def tabulate_pair(r, carry):
        tabulate(0, r)
        tabulate(1, r)
        return carry

    lax.fori_loop(0, pairs, tabulate_pair, 0)

    values = tokens_ref[...].astype(F32)
    scale = lax.rsqrt(jnp.mean(values * values, axis=-1, keepdims=True) + epsilon)
    normed = (values * scale * norm_ref[...]).astype(BF16)
    loads[1].wait()
    for load in loads[2:]:
        load.start()
    driven = jnp.dot(normed, in_ref[...], preferred_element_type=F32).astype(BF16)
    driven_ref[...] = jnp.dot(permute, driven, preferred_element_type=F32).astype(BF16)

    lane = lax.broadcasted_iota(jnp.int32, (1, LANES), 1)

    def unit(k, r, dec_ref, proj_ref):
        state = prod = None
        order = range(steps) if k == 0 else range(steps - 1, -1, -1)
        for j in order:
            at = slice(j * SUB, (j + 1) * SUB)
            decay = (
                dec_ref[at, k * 256 : k * 256 + 128], dec_ref[at, k * 256 + 128 : k * 256 + 256]
            )
            damping = dec_ref[at, 512 + k * 128 : 640 + k * 128]
            push_re = proj_ref[at, k * 256 : k * 256 + 128] * damping
            push_im = proj_ref[at, k * 256 + 128 : k * 256 + 256] * damping
            if state is None:
                state, prod = (push_re, push_im), decay
            else:
                moved = cmul(decay, state)
                state = (moved[0] + push_re, moved[1] + push_im)
                prod = cmul(decay, prod)
            sre[k, r, at, :] = state[0]
            sim[k, r, at, :] = state[1]
            pre[k, r, at, :] = prod[0]
            pim[k, r, at, :] = prod[1]
        ends[k, 0, r] = state[0]
        ends[k, 1, r] = state[1]
        ends[k, 2, r] = prod[0]
        ends[k, 3, r] = prod[1]

    def block(b, carry):
        start = pl.multiple_of(b * LANES, LANES)
        piece = driven_ref[:, pl.ds(start, LANES)]
        spread(drive_raw, drive_ref, start, 0, False)
        weight = drive_ref[...]

        for i in range(inner):
            r = b * inner + i
            mask = (lane // wide == i).astype(F32).astype(BF16)
            proj_ref[i] = jnp.dot(piece * mask, weight, preferred_element_type=F32)
            dec_ref[i, :, :512] = jnp.dot(
                basis, rhs_ref[r, :, :512], preferred_element_type=F32
            )
            dec_ref[i, :, 512:] = jnp.dot(
                rooted, rhs_ref[r, :, 512:], preferred_element_type=F32
            )
            unit(0, r, dec_ref.at[i], proj_ref.at[i])
            unit(1, r, dec_ref.at[i], proj_ref.at[i])
        return carry

    loads[0].wait()
    lax.fori_loop(0, blocks, block, 0)

    sub = lax.broadcasted_iota(jnp.int32, (per, SUB, LANES), 1)
    for q in range(tp_size):
        for k in range(2):
            at = slice(q * per, (q + 1) * per)
            s = (ends[k, 0, at], ends[k, 1, at])
            p = (ends[k, 2, at], ends[k, 3, at])

            def shift(x, far, fill):
                moved = pltpu.roll(x, far if k == 0 else SUB - far, 1)
                keep = sub >= far if k == 0 else sub < SUB - far
                return jnp.where(keep, moved, fill)

            for far in (1, 2, 4):
                old_s = (shift(s[0], far, 0.0), shift(s[1], far, 0.0))
                old_p = (shift(p[0], far, 1.0), shift(p[1], far, 0.0))
                moved = cmul(p, old_s)
                s = (moved[0] + s[0], moved[1] + s[1])
                p = cmul(p, old_p)
            last = SUB - 1 if k == 0 else 0
            send1[q, 2 * k] = s[0][:, last, :]
            send1[q, 2 * k + 1] = s[1][:, last, :]
            segs[k, 0, at] = shift(s[0], 1, 0.0)
            segs[k, 1, at] = shift(s[1], 1, 0.0)
            segs[k, 2, at] = shift(p[0], 1, 1.0)
            segs[k, 3, at] = shift(p[1], 1, 0.0)
        send1[q, 4] = jnp.broadcast_to(total_time, (per, LANES))

    pl.semaphore_wait(barrier, tp_size + sp_size - 2)

    def exchange_tp(send, recv, ssem, rsem, meanwhile=None):
        outs = []
        for off in range(1, tp_size):
            peer = lax.rem(my_tp + off, tp_size)
            copy = pltpu.make_async_remote_copy(
                src_ref=send.at[peer], dst_ref=recv.at[my_tp],
                send_sem=ssem.at[peer], recv_sem=rsem.at[my_tp],
                device_id=(my_sp, peer), device_id_type=pl.DeviceIdType.MESH,
            )
            copy.start()
            outs.append(copy)
        recv[my_tp] = send[my_tp]
        if meanwhile is not None:
            meanwhile()
        for off in range(1, tp_size):
            peer = lax.rem(my_tp + off, tp_size)
            pltpu.make_async_remote_copy(
                src_ref=send.at[peer], dst_ref=recv.at[peer],
                send_sem=ssem.at[peer], recv_sem=rsem.at[peer],
                device_id=(my_sp, peer), device_id_type=pl.DeviceIdType.MESH,
            ).wait_recv()
        return outs

    def prepare_read():
        loads[2].wait()

        def piece(b, carry):
            start = pl.multiple_of(b * LANES, LANES)
            spread(read_raw, read_ref, start, start, True)
            return carry

        lax.fori_loop(0, blocks, piece, 0)

    pending = exchange_tp(send1, recv1, s1s, r1s, prepare_read)
    mine = pl.ds(my_tp * per, per)
    rate = (rate_ref[0, mine, :], rate_ref[1, mine, :])
    angle = (angle_ref[0, mine, :], angle_ref[1, mine, :])
    fold = []
    for k in range(2):
        fold.append([decay_of(rate[k], angle[k], recv1[i, 4]) for i in range(tp_size)])
    group_time = recv1[0, 4]
    for i in range(1, tp_size):
        group_time = group_time + recv1[i, 4]
    for k in range(2):
        total = None
        for i in range(tp_size) if k == 0 else range(tp_size - 1, -1, -1):
            s = (recv1[i, 2 * k], recv1[i, 2 * k + 1])
            if total is None:
                total = s
            else:
                moved = cmul(fold[k][i], total)
                total = (moved[0] + s[0], moved[1] + s[1])
        send2[2 * k] = total[0]
        send2[2 * k + 1] = total[1]
    send2[4] = group_time

    for off in range(1, sp_size):
        peer = lax.rem(my_sp + off, sp_size)
        copy = pltpu.make_async_remote_copy(
            src_ref=send2, dst_ref=recv2.at[my_sp],
            send_sem=s2s.at[peer], recv_sem=r2s.at[my_sp],
            device_id=(peer, my_tp), device_id_type=pl.DeviceIdType.MESH,
        )
        copy.start()
        pending.append(copy)
    recv2[my_sp] = send2[...]
    for off in range(1, sp_size):
        peer = lax.rem(my_sp + off, sp_size)
        pltpu.make_async_remote_copy(
            src_ref=send2, dst_ref=recv2.at[peer],
            send_sem=s2s.at[peer], recv_sem=r2s.at[peer],
            device_id=(peer, my_tp), device_id_type=pl.DeviceIdType.MESH,
        ).wait_recv()

    for k in range(2):
        enter = (jnp.zeros((per, LANES), F32), jnp.zeros((per, LANES), F32))
        for i in range(sp_size) if k == 0 else range(sp_size - 1, -1, -1):
            moved = cmul(decay_of(rate[k], angle[k], recv2[i, 4]), enter)
            reached = (jnp.full((per, LANES), i, jnp.int32) < my_sp) if k == 0 else (
                jnp.full((per, LANES), i, jnp.int32) > my_sp
            )
            enter = tuple(
                jnp.where(reached, moved[c] + recv2[i, 2 * k + c], enter[c]) for c in range(2)
            )
        for i in range(tp_size) if k == 0 else range(tp_size - 1, -1, -1):
            send3[i, 2 * k] = enter[0]
            send3[i, 2 * k + 1] = enter[1]
            moved = cmul(fold[k][i], enter)
            enter = tuple(moved[c] + recv1[i, 2 * k + c] for c in range(2))
    pending = pending + exchange_tp(send3, recv3, s3s, r3s)

    def read_block(b, carry):
        start = pl.multiple_of(b * LANES, LANES)
        weight = read_ref[pl.ds(start, LANES), :]

        def one(i):
            r = b * inner + i
            q, row = r // per, lax.rem(r, per)
            for k in range(2):
                enter = (
                    recv3[q, 2 * k, pl.ds(row, 1), :],
                    recv3[q, 2 * k + 1, pl.ds(row, 1), :],
                )
                moved = cmul((segs[k, 2, r], segs[k, 3, r]), enter)
                enter = (moved[0] + segs[k, 0, r], moved[1] + segs[k, 1, r])
                shape = (steps, SUB, LANES)
                prod = (pre[k, r].reshape(shape), pim[k, r].reshape(shape))
                moved = cmul(prod, enter)
                whole_re = sre[k, r].reshape(shape) + moved[0]
                whole_im = sim[k, r].reshape(shape) + moved[1]
                st_ref[i, :, k * 256 : k * 256 + 128] = whole_re.reshape(rows, LANES).astype(BF16)
                st_ref[i, :, k * 256 + 128 : k * 256 + 256] = whole_im.reshape(rows, LANES).astype(BF16)
            out = lax.dot_general(
                st_ref[i], weight, (((1,), (1,)), ((), ())), preferred_element_type=F32
            )
            return jnp.where(lane // wide == i, out, 0.0)

        total = one(0)
        for i in range(1, inner):
            total = total + one(i)
        resp_ref[:, pl.ds(start, LANES)] = total
        return carry

    lax.fori_loop(0, blocks, read_block, 0)

    response = resp_ref[...] + skip_ref[...] * driven_ref[...].astype(F32)
    active = jax.nn.gelu(response)
    loads[3].wait()
    gate = jnp.dot(active.astype(BF16), glu_ref[...], preferred_element_type=F32) + bias_ref[...]
    gated = (active * jax.nn.sigmoid(gate)).astype(BF16)
    gated = jnp.dot(back, gated, preferred_element_type=F32).astype(BF16)
    loads[4].wait()
    projected = jnp.dot(gated, out_ref[...], preferred_element_type=F32)
    scale = lax.rsqrt(jnp.mean(projected * projected, axis=-1, keepdims=True) + epsilon)
    mixed_ref[...] = (projected * scale * gain_ref[...]).astype(BF16)
    for copy in pending:
        copy.wait_send()


def local(
    sp_size, tp_size, tokens, elapsed, norm_gain, in_weight, state_input, state_output,
    forget_rate, decay_angle, skip_gain, glu_weight, glu_bias, out_weight, out_gain,
):
    rows, width = tokens.shape
    channels = in_weight.shape[1]
    _, _, groups, states, _ = state_input.shape
    share = LANES // states
    pairs = groups // share
    per = pairs // tp_size
    inner = pairs // (channels // LANES)
    drive = state_input.transpose(0, 1, 2, 4, 3).reshape(2, 2, channels, states)
    read = state_output.reshape(2, 2, channels, states)
    turns = np.pi * (np.arange(LANES) % NODES + 0.5) / NODES
    orders = np.arange(NODES)[:, None]
    basis = np.cos(orders * turns[None, :]) * np.where(orders == 0, 1, 2) / NODES
    nodes = np.broadcast_to((np.cos(turns[:NODES, None]) + 1) * (SPAN / 2), (NODES, LANES))

    vmem = pl.BlockSpec(memory_space=pltpu.VMEM)
    hbm = pl.BlockSpec(memory_space=pl.ANY)
    cells = (2, pairs, rows, LANES)
    dma = pltpu.SemaphoreType.DMA
    return pl.pallas_call(
        functools.partial(kernel, sp_size, tp_size),
        out_shape=jax.ShapeDtypeStruct((rows, width), BF16),
        in_specs=[vmem] * 10 + [hbm] * 5,
        out_specs=vmem,
        scratch_shapes=[
            pltpu.VMEM(drive.shape, BF16),
            pltpu.VMEM(in_weight.shape, BF16),
            pltpu.VMEM(read.shape, F32),
            pltpu.VMEM(glu_weight.shape, BF16),
            pltpu.VMEM(out_weight.shape, BF16),
            pltpu.VMEM((2, pairs, LANES), F32),
            pltpu.VMEM((2, pairs, LANES), F32),
            pltpu.VMEM((LANES, 4 * LANES), BF16),
            pltpu.VMEM((channels, 4 * LANES), BF16),
            pltpu.VMEM((pairs, LANES, 6 * LANES), BF16),
            pltpu.VMEM((inner, rows, 6 * LANES), F32),
            pltpu.VMEM((rows, channels), BF16),
            pltpu.VMEM((inner, rows, 4 * LANES), F32),
            pltpu.VMEM(cells, F32),
            pltpu.VMEM(cells, F32),
            pltpu.VMEM(cells, F32),
            pltpu.VMEM(cells, F32),
            pltpu.VMEM((2, 4, pairs, SUB, LANES), F32),
            pltpu.VMEM((2, 4, pairs, SUB, LANES), F32),
            pltpu.VMEM((inner, rows, 4 * LANES), BF16),
            pltpu.VMEM((rows, channels), F32),
            pltpu.VMEM((tp_size, 5, per, LANES), F32),
            pltpu.VMEM((tp_size, 5, per, LANES), F32),
            pltpu.VMEM((5, per, LANES), F32),
            pltpu.VMEM((sp_size, 5, per, LANES), F32),
            pltpu.VMEM((tp_size, 4, per, LANES), F32),
            pltpu.VMEM((tp_size, 4, per, LANES), F32),
            dma((5,)),
            dma((tp_size,)),
            dma((tp_size,)),
            dma((sp_size,)),
            dma((sp_size,)),
            dma((tp_size,)),
            dma((tp_size,)),
        ],
        compiler_params=pltpu.CompilerParams(
            collective_id=0, has_side_effects=True, vmem_limit_bytes=60 * 1024 * 1024
        ),
    )(
        tokens, elapsed.reshape(1, rows), norm_gain.reshape(1, -1), forget_rate, decay_angle,
        skip_gain.reshape(1, -1), glu_bias.reshape(1, -1), out_gain.reshape(1, -1),
        jnp.asarray(basis, F32), jnp.asarray(nodes, F32),
        drive, in_weight, read, glu_weight, out_weight,
    )


def solution(mesh):
    rows = P(("sp", "tp"), None)
    return jax.shard_map(
        functools.partial(local, mesh.shape["sp"], mesh.shape["tp"]),
        mesh=mesh,
        in_specs=(rows, P(("sp", "tp"))) + (P(),) * 11,
        out_specs=rows,
        check_vma=False,
    )
```
